32 devices in a mesh: kv: 8 (over z, y), tp: 4 (over x, core).
Axes of the slice: x: 2, y: 2, z: 4, core: 2. Of those that a mesh axis runs over, the one named last changes fastest.
Arguments:
- tokens: bfloat16 [16, 4096], P(None, 'kv')
- norm_gain: float32 [4096], P('kv'), may hold values from 0.1 to 1.9
- w_query: bfloat16 [4096, 3072], P('kv', 'tp'), may hold values from -0.09375 to 0.09375
- w_key: bfloat16 [4096, 3072], P('kv', 'tp'), may hold values from -0.09375 to 0.09375
- w_value: bfloat16 [4096, 3072], P('kv', 'tp'), may hold values from -0.09375 to 0.09375
- w_forget: bfloat16 [4096, 48], P('kv'), may hold values from -0.09375 to 0.09375
- w_out: bfloat16 [3072, 4096], P('tp', 'kv'), may hold values from -0.109375 to 0.109375
- mix_gain: float32 [4096], P('kv'), may hold values from 0.1 to 1.9
- w_up: bfloat16 [4096, 16384], P('kv', 'tp'), may hold values from -0.09375 to 0.09375
- w_down: bfloat16 [16384, 4096], P('tp', 'kv'), may hold values from -0.0625 to 0.0625
- key_cache: bfloat16 [16, 1024, 3072], P(None, 'kv', 'tp')
- value_cache: bfloat16 [16, 1024, 3072], P(None, 'kv', 'tp'), may hold values from -6 to 6
- decay_cache: float32 [16, 48, 1024], P(None, 'tp', 'kv')
- lengths: int32 [16], replicated, may hold values from 1 to 1024, 5461 in all
Outputs:
- layer_out: bfloat16 [16, 4096], P(None, 'kv')
The draws below stay inside these ranges and needn't reach their ends.
Inputs may be any that keep to these rules, and one draw needn't show every extreme that they name: `lengths`: one sequence fills all 1024 positions.
All inputs are finite; a program needn't handle non-finite values.
Results may differ from the reference program's by a relative error of at most 0.01.
Values may be sent and summed in bfloat16 or wider, within the bound.
A program may use at most 64 MiB of HBM per device.

```python
import math
import jax
import jax.numpy as jnp
import numpy as np
from jax import lax

D = 4096
ATTENTION_HEADS = 48
HEAD_DIM = 64
FF = 16384
BATCH_SEQUENCES = 16
POS_DEV = 128
ATT = 3072
CACHE_CAPACITY = 1024


def draw_tokens(key, part):
    flow_lanes = jax.random.split(jax.random.fold_in(key, 3), 2)
    columns = jnp.arange(D, dtype=jnp.float32)
    column_scale = 10.0 ** (columns / D)
    row_factor = jnp.exp(jax.random.uniform(flow_lanes[0], (BATCH_SEQUENCES, 1), jnp.float32, 0.0, jnp.log(4.0)))
    sample = jax.random.normal(flow_lanes[1], (BATCH_SEQUENCES, D), jnp.float32)
    return (sample * column_scale * row_factor / 5.0).astype(jnp.bfloat16)


def draw_key_cache(key, part):
    flow_lanes = jax.random.split(jax.random.fold_in(key, 5), 1)
    sample = jax.random.normal(flow_lanes[0], (BATCH_SEQUENCES, CACHE_CAPACITY, ATT), jnp.float32)
    return sample.astype(jnp.bfloat16)


def draw_value_cache(key, part):
    flow_lanes = jax.random.split(jax.random.fold_in(key, 11), 3)
    block_count = CACHE_CAPACITY // POS_DEV
    channel_mean = jax.random.uniform(flow_lanes[0], (BATCH_SEQUENCES, 1, 1, ATT), jnp.float32, -2.0, 2.0)
    block_offset = jax.random.uniform(flow_lanes[1], (BATCH_SEQUENCES, block_count, 1, ATT), jnp.float32, -1.5, 1.5)
    noise = jax.random.normal(flow_lanes[2], (BATCH_SEQUENCES, block_count, POS_DEV, ATT), jnp.float32)
    sample = jnp.clip(channel_mean + block_offset + noise, -6.0, 6.0)
    return sample.reshape(BATCH_SEQUENCES, CACHE_CAPACITY, ATT).astype(jnp.bfloat16)


def draw_decay_cache(key, part):
    flow_lanes = jax.random.split(jax.random.fold_in(key, 7), 7)
    slow_share = 0.5
    gradual_heads = (jax.random.uniform(flow_lanes[0], (BATCH_SEQUENCES, ATTENTION_HEADS, 1), jnp.float32) < slow_share).astype(jnp.float32)
    slow_rate = jax.random.uniform(flow_lanes[1], (BATCH_SEQUENCES, ATTENTION_HEADS, 1), jnp.float32, 0.3, 0.8) / CACHE_CAPACITY
    fast_rate = jax.random.uniform(flow_lanes[2], (BATCH_SEQUENCES, ATTENTION_HEADS, 1), jnp.float32, 0.02, 0.035)
    decay_rates = gradual_heads * slow_rate + (1.0 - gradual_heads) * fast_rate
    block_count = CACHE_CAPACITY // POS_DEV
    block_multiplier = jnp.exp(jax.random.uniform(flow_lanes[3], (BATCH_SEQUENCES, ATTENTION_HEADS, block_count, 1), jnp.float32, jnp.log(0.4), jnp.log(2.5)))
    block_multiplier = jnp.broadcast_to(block_multiplier, (BATCH_SEQUENCES, ATTENTION_HEADS, block_count, POS_DEV)).reshape(BATCH_SEQUENCES, ATTENTION_HEADS, CACHE_CAPACITY)
    jaggedness = jax.random.uniform(flow_lanes[4], (BATCH_SEQUENCES, ATTENTION_HEADS, CACHE_CAPACITY), jnp.float32, 0.5, 1.5)
    spike_events = (jax.random.uniform(flow_lanes[5], (BATCH_SEQUENCES, ATTENTION_HEADS, CACHE_CAPACITY), jnp.float32) < 3.0 / CACHE_CAPACITY).astype(jnp.float32)
    spike_removal = jax.random.uniform(flow_lanes[6], (BATCH_SEQUENCES, ATTENTION_HEADS, CACHE_CAPACITY), jnp.float32, 0.22, 0.69)
    forget_gates = -decay_rates * block_multiplier * jaggedness - spike_events * spike_removal * gradual_heads
    return jnp.cumsum(forget_gates, axis=2)


def steps_of(stream_key, dims, cuts, smallest, largest):
    loudness = 1.0
    for dim, parts in cuts:
        heights = jax.random.uniform(jax.random.fold_in(jax.random.fold_in(stream_key, 6), dim), (parts,), jnp.float32, smallest / len(cuts), largest / len(cuts))
        loudness = loudness * jnp.repeat(jnp.exp(heights), dims[dim] // parts).reshape((-1,) + (1,) * (len(dims) - 1 - dim))
    return loudness


def split_up(number_of, total, limit, skew):
    loads = [(1 << 20) // math.isqrt(standing ** skew) + 1 for standing in range(2, number_of + 1)]
    spare, counts = total - limit - (number_of - 1), [1] * (number_of - 1)
    while spare > 0:
        movable = [i for i in range(number_of - 1) if counts[i] < limit]
        whole, left = sum([loads[i] for i in movable]), spare
        for i in movable:
            more = min(limit - counts[i], max(1, left * loads[i] // whole), spare)
            counts[i] = counts[i] + more
            spare = spare - more
    return np.array([limit] + counts)


def ragged_sizes(rng, number_of, total, limit, slope):
    if number_of == 2:
        one = jax.random.randint(rng, (), max(1, total - limit), min(limit, total - 1) + 1)
        return jnp.stack([one, total - one])
    sizes = jnp.asarray(split_up(number_of, total, limit, slope), jnp.int32)
    twos = (number_of - 1) // 2
    giver, receiver = sizes[1:1 + 2 * twos:2], sizes[2:2 + 2 * twos:2]
    margin = jnp.minimum(giver - 1, limit - receiver)
    shifted = jax.random.randint(jax.random.fold_in(rng, 1), (twos,), 0, 1 << 20) % (margin + 1)
    sizes = sizes.at[1:1 + 2 * twos:2].set(giver - shifted).at[2:2 + 2 * twos:2].set(receiver + shifted)
    return sizes[jax.random.permutation(jax.random.fold_in(rng, 2), number_of)]


def gaussian(stream_key, extent, deviation, limit, pieces=(), kind=jnp.bfloat16):
    gain = steps_of(stream_key, extent, pieces, -0.22, 0.18) if pieces else 1.0
    values = jax.random.normal(stream_key, extent, jnp.float32) * deviation * gain
    return jnp.minimum(jnp.maximum(values, -limit), limit).astype(kind)


def setup_inputs(seed: int = 0) -> dict:
    seeds = jax.random.split(jax.random.key(seed), 15)
    tokens = draw_tokens(jax.random.fold_in(seeds[14], 71), 0)
    norm_gain = jnp.clip(1.0 + 0.18 * jax.random.normal(seeds[1], (D,), jnp.float32), 0.1, 1.9)
    w_query = gaussian(seeds[2], (D, ATT), D ** -0.5, 0.09375, ((0, 8), (1, 4)))
    w_key = gaussian(seeds[3], (D, ATT), D ** -0.5, 0.09375, ((0, 8), (1, 4)))
    w_value = gaussian(seeds[4], (D, ATT), D ** -0.5, 0.09375, ((0, 8), (1, 4)))
    w_forget = gaussian(seeds[5], (D, ATTENTION_HEADS), D ** -0.5, 0.09375, ((0, 8),))
    w_out = gaussian(seeds[6], (ATT, D), ATT ** -0.5, 0.109375, ((0, 4), (1, 8)))
    mix_gain = jnp.clip(1.0 + 0.18 * jax.random.normal(seeds[7], (D,), jnp.float32), 0.1, 1.9)
    w_up = gaussian(seeds[8], (D, FF), D ** -0.5, 0.09375, ((0, 8), (1, 4)))
    w_down = gaussian(seeds[9], (FF, D), (FF // 2) ** -0.5, 0.0625, ((0, 4), (1, 8)))
    key_cache = draw_key_cache(jax.random.fold_in(seeds[14], 71), 0)
    value_cache = draw_value_cache(jax.random.fold_in(seeds[14], 71), 0)
    decay_cache = draw_decay_cache(jax.random.fold_in(seeds[14], 71), 0)
    lengths = ragged_sizes(seeds[13], BATCH_SEQUENCES, BATCH_SEQUENCES * CACHE_CAPACITY // 3, CACHE_CAPACITY, 2).astype(jnp.int32)
    return {"tokens": tokens, "norm_gain": norm_gain, "w_query": w_query, "w_key": w_key, "w_value": w_value, "w_forget": w_forget, "w_out": w_out, "mix_gain": mix_gain, "w_up": w_up, "w_down": w_down, "key_cache": key_cache, "value_cache": value_cache, "decay_cache": decay_cache, "lengths": lengths}


epsilon = 1e-06
very_low = -1e+30

def block_softmax(query_heads, score_bias, keys_block, values_block, live_mask):
    rows_count, count = (keys_block.shape[0], keys_block.shape[1])
    heads_count = query_heads.shape[1]
    keys_float = keys_block.astype(jnp.float32).reshape(rows_count, count, heads_count, HEAD_DIM)
    values_float = values_block.astype(jnp.float32).reshape(rows_count, count, heads_count, HEAD_DIM)
    scores = jnp.einsum('bhe,bphe->bhp', query_heads, keys_float) * HEAD_DIM ** (-0.5) + score_bias
    block_peak = lax.optimization_barrier(jnp.max(jnp.where(live_mask, scores, very_low), axis=2))
    weights = jnp.where(live_mask, jnp.exp(scores - block_peak[..., None]), 0.0)
    totals = lax.optimization_barrier(jnp.sum(weights, axis=2))
    rounded = lax.optimization_barrier(weights.astype(jnp.bfloat16)).astype(jnp.float32)
    weighted = jnp.einsum('bhp,bphe->bhe', rounded, values_float)
    return (block_peak, totals, weighted)

def join(earlier, later_part):
    highest = jnp.maximum(earlier[0], later_part[0])
    factor_one = jnp.exp(earlier[0] - highest)
    factor_two = jnp.exp(later_part[0] - highest)
    totals = earlier[1] * factor_one + later_part[1] * factor_two
    weighted = earlier[2] * factor_one[..., None] + later_part[2] * factor_two[..., None]
    return (highest, totals, weighted)

def reference(tokens, norm_gain, w_query, w_key, w_value, w_forget, w_out, mix_gain, w_up, w_down, key_cache, value_cache, decay_cache, lengths):
    rows_count = tokens.shape[0]
    tokens_f = tokens.astype(jnp.float32)
    row_scale = lax.rsqrt(lax.optimization_barrier(jnp.mean(tokens_f * tokens_f, axis=1)) + epsilon)[:, None]
    scaled_in = (tokens_f * norm_gain.astype(jnp.float32)).astype(jnp.bfloat16)
    queries = (row_scale * jnp.dot(scaled_in, w_query, preferred_element_type=jnp.float32)).astype(jnp.bfloat16)
    new_keys = (row_scale * jnp.dot(scaled_in, w_key, preferred_element_type=jnp.float32)).astype(jnp.bfloat16)
    new_values = (row_scale * jnp.dot(scaled_in, w_value, preferred_element_type=jnp.float32)).astype(jnp.bfloat16)
    log_forget = jax.nn.log_sigmoid(row_scale * jnp.dot(scaled_in, w_forget, preferred_element_type=jnp.float32))
    positions = jnp.arange(CACHE_CAPACITY, dtype=jnp.int32)
    newest = positions[None, None, :] == (lengths - 1)[:, None, None]
    now_decay = lax.optimization_barrier(jnp.sum(jnp.where(newest, decay_cache, 0.0), axis=2)) + log_forget
    query_heads = queries.astype(jnp.float32).reshape(rows_count, ATTENTION_HEADS, HEAD_DIM)
    own_keys = new_keys.astype(jnp.float32).reshape(rows_count, ATTENTION_HEADS, HEAD_DIM)
    own_score = lax.optimization_barrier(jnp.sum(query_heads * own_keys, axis=2)) * HEAD_DIM ** (-0.5)
    start_state = (own_score, jnp.ones_like(own_score), new_values.astype(jnp.float32).reshape(rows_count, ATTENTION_HEADS, HEAD_DIM))

    def visit(carried, block_index):
        offset = block_index * POS_DEV
        keys_block = lax.dynamic_slice_in_dim(key_cache, offset, POS_DEV, 1)
        values_block = lax.dynamic_slice_in_dim(value_cache, offset, POS_DEV, 1)
        decay_block = lax.dynamic_slice_in_dim(decay_cache, offset, POS_DEV, 2)
        live_mask = (offset + jnp.arange(POS_DEV, dtype=jnp.int32))[None, None, :] < lengths[:, None, None]
        piece_state = block_softmax(query_heads, now_decay[:, :, None] - decay_block, keys_block, values_block, live_mask)
        return (join(carried, piece_state), None)
    final_state, unused = lax.scan(visit, start_state, jnp.arange(CACHE_CAPACITY // POS_DEV, dtype=jnp.int32))
    attended = (final_state[2] / final_state[1][..., None]).reshape(rows_count, ATTENTION_HEADS * HEAD_DIM).astype(jnp.bfloat16)
    mixed_in = (tokens_f + jnp.dot(attended, w_out, preferred_element_type=jnp.float32)).astype(jnp.bfloat16)
    mixed_f = mixed_in.astype(jnp.float32)
    mix_scale = lax.rsqrt(lax.optimization_barrier(jnp.mean(mixed_f * mixed_f, axis=1)) + epsilon)[:, None]
    mix_in = (mixed_f * mix_gain.astype(jnp.float32)).astype(jnp.bfloat16)
    upward = mix_scale * jnp.dot(mix_in, w_up, preferred_element_type=jnp.float32)
    hidden = (jax.nn.relu(upward) ** 2).astype(jnp.bfloat16)
    return (mixed_f + jnp.dot(hidden, w_down, preferred_element_type=jnp.float32)).astype(jnp.bfloat16)
```

```python
import functools

import jax
import jax.numpy as jnp
from jax import lax
from jax.experimental import pallas as pl
from jax.experimental.pallas import tpu as pltpu
from jax.sharding import PartitionSpec as P

HEAD_DIM = 64

epsilon = 1e-06
very_low = -1e30
LANES = 128
F32 = jnp.float32
BF16 = jnp.bfloat16

EX_Q, EX_SMALL, EX_KV, EX_O, EX_LSE, EX_OUT, EX_UP, EX_SQ, EX_HID, EX_DOWN = range(10)
LANE_NEWEST = 32
LANE_SQUARES = 64


def mm(a, b):
    return jnp.dot(a, b, preferred_element_type=F32)


def split_mm(a, b):
    high = a.astype(BF16)
    low = (a - high.astype(F32)).astype(BF16)
    return mm(high, b) + mm(low, b)


def mm_t(a, spread):
    return lax.dot_general(a, spread, (((1,), (1,)), ((), ())), preferred_element_type=F32)


def layer_kernel(
    n_kv,
    n_tp,
    lengths,
    tokens_h,
    gain_h,
    wq_h,
    wk_h,
    wv_h,
    wf_h,
    wo_h,
    mix_gain_h,
    wu_h,
    wd_h,
    kc_h,
    vc_h,
    decay_h,
    out_h,
    tokens_v,
    gain_v,
    wq,
    wk,
    wv,
    wf,
    wo,
    mix_gain_v,
    wu,
    wd,
    kc,
    vc,
    decay,
    q_all,
    small_all,
    kv_send,
    kv_all,
    q_s,
    bias_s,
    base_s,
    now_s,
    o_s,
    lse_s,
    o_all,
    lse_all,
    out_all,
    up_send,
    up_all,
    sq_all,
    hid_all,
    down_all,
    load_sem,
    send_sem,
    recv_sem,
):
    j = lax.axis_index("kv")
    t = lax.axis_index("tp")
    rows, feats = tokens_v.shape
    width = feats * n_kv
    att = wq.shape[1]
    heads = decay.shape[0]
    span = decay.shape[2]
    own_rows = rows // n_kv
    chunk = wu.shape[1] // n_kv

    loads = [
        pltpu.make_async_copy(src, dst, load_sem.at[i])
        for i, (src, dst) in enumerate(
            [
                (tokens_h, tokens_v),
                (gain_h, gain_v),
                (wf_h, wf),
                (wq_h, wq),
                (decay_h, decay),
                (wk_h, wk),
                (wv_h, wv),
                (kc_h, kc),
                (vc_h, vc),
                (wo_h, wo),
                (mix_gain_h, mix_gain_v),
                (wu_h, wu),
                (wd_h, wd),
            ]
        )
    ]
    names = ("tok", "gain", "wf", "wq", "decay", "wk", "wv", "kc", "vc", "wo", "mg", "wu", "wd")
    L = dict(zip(names, loads))
    barrier = pltpu.get_barrier_semaphore()
    for k in range(1, n_kv):
        pl.semaphore_signal(
            barrier, inc=1, device_id={"kv": lax.rem(j + k, n_kv)}, device_id_type=pl.DeviceIdType.MESH
        )
    for k in range(1, n_tp):
        pl.semaphore_signal(
            barrier, inc=1, device_id={"tp": lax.rem(t + k, n_tp)}, device_id_type=pl.DeviceIdType.MESH
        )

    for name in names[:5]:
        L[name].start()

    def copy(ex, src, dst, axis, peer, me):
        return pltpu.make_async_remote_copy(
            src_ref=src,
            dst_ref=dst,
            send_sem=send_sem.at[ex, peer],
            recv_sem=recv_sem.at[ex, me],
            device_id={axis: peer},
            device_id_type=pl.DeviceIdType.MESH,
        )

    sent = []

    def send(ex, src, dst, axis, peer, me):
        c = copy(ex, src, dst, axis, peer, me)
        c.start()
        sent.append(c)

    def arrived(ex, buf, axis, peer):
        copy(ex, buf.at[peer], buf.at[peer], axis, peer, peer).wait_recv()

    kv_peers = [lax.rem(j + k, n_kv) for k in (4, 3, 5, 2, 6, 1, 7)] if n_kv == 8 else [
        lax.rem(j + k, n_kv) for k in range(1, n_kv)
    ]
    tp_peers = [lax.rem(t + k, n_tp) for k in range(1, n_tp)]

    lane = lax.broadcasted_iota(jnp.int32, (heads, LANES), 1)
    sub = lax.broadcasted_iota(jnp.int32, (heads, LANES), 0)
    eye = lane == sub
    eye_newest = lane == sub + LANE_NEWEST
    head_mask = (
        lax.broadcasted_iota(jnp.int32, (heads, att), 1) // HEAD_DIM
        == lax.broadcasted_iota(jnp.int32, (heads, att), 0)
    )
    spread = (
        lax.broadcasted_iota(jnp.int32, (LANES, att), 1) // HEAD_DIM
        == lax.broadcasted_iota(jnp.int32, (LANES, att), 0)
    ).astype(F32).astype(BF16)
    position = lax.broadcasted_iota(jnp.int32, (heads, span), 1) + j * span
    lane_r = lax.broadcasted_iota(jnp.int32, (rows, LANES), 1)

    L["tok"].wait()
    L["gain"].wait()
    tokens_f = tokens_v[...].astype(F32)
    scaled_in = (tokens_f * gain_v[...]).astype(BF16)
    squares = jnp.sum(tokens_f * tokens_f, axis=1, keepdims=True)
    L["wf"].wait()
    forget = mm_t(scaled_in, wf[...])
    mine = forget[:, 0:heads]
    for k in range(1, n_tp):
        mine = jnp.where(t == k, forget[:, k * heads : (k + 1) * heads], mine)
    L["wq"].wait()
    for name in names[5:]:
        L[name].start()
    q_all[j] = mm(scaled_in, wq[...]).astype(BF16)
    L["decay"].wait()
    for b in range(rows):
        fall = decay[:, b, :]
        hit = jnp.sum(jnp.where(position == lengths[b] - 1, fall, 0.0), axis=1, keepdims=True)
        now_s[b : b + 1, :] = jnp.sum(jnp.where(eye_newest, hit, 0.0), axis=0, keepdims=True)
    small_all[j] = now_s[...] + jnp.where(lane_r == LANE_SQUARES, squares, 0.0)
    small_all[j, :, 0:heads] = mine

    pl.semaphore_wait(barrier, n_kv - 1 + n_tp - 1)
    for d in kv_peers:
        send(EX_Q, q_all.at[j], q_all.at[j], "kv", d, j)
        send(EX_SMALL, small_all.at[j], small_all.at[j], "kv", d, j)
    L["wk"].wait()
    new_k = mm(scaled_in, wk[...])
    L["wv"].wait()
    new_v = mm(scaled_in, wv[...])
    for d in range(n_kv):
        kv_send[d, :, 0:att] = new_k[d * own_rows : (d + 1) * own_rows].astype(BF16)
        kv_send[d, :, att:] = new_v[d * own_rows : (d + 1) * own_rows].astype(BF16)
    kv_all[j] = kv_send[j]
    for d in kv_peers:
        send(EX_KV, kv_send.at[d], kv_all.at[j], "kv", d, j)

    for b in range(rows):
        fall = decay[:, b, :]
        base = fall[:, 0:1]
        bias_s[b] = jnp.where(position < lengths[b], base - fall, very_low)
        base_s[b : b + 1, :] = jnp.sum(jnp.where(eye, base, 0.0), axis=0, keepdims=True)

    for d in reversed(kv_peers):
        arrived(EX_SMALL, small_all, "kv", d)
        arrived(EX_Q, q_all, "kv", d)
    small = jnp.sum(small_all[...], axis=0)
    row_scale = lax.rsqrt(small[:, LANE_SQUARES : LANE_SQUARES + 1] / width + epsilon)
    gate = row_scale * small[:, 0:heads]
    log_forget = jnp.minimum(gate, 0.0) - jnp.log1p(jnp.exp(-jnp.abs(gate)))
    now_s[...] = jnp.zeros_like(now_s)
    now_s[:, 0:heads] = small[:, LANE_NEWEST : LANE_NEWEST + heads] + log_forget
    q_sum = q_all[0].astype(F32)
    for d in range(1, n_kv):
        q_sum += q_all[d].astype(F32)
    q_s[...] = (row_scale * q_sum).astype(BF16).astype(F32)

    L["kc"].wait()
    scores = []
    for b in range(rows):
        query = jnp.where(head_mask, q_s[b : b + 1, :], 0.0).astype(BF16)
        scores.append(mm_t(query, kc[b]))
    weights = []
    inverse = []
    for b in range(rows):
        live = position < lengths[b]
        s = jnp.where(live, scores[b] * HEAD_DIM ** (-0.5) + bias_s[b], very_low)
        peak = jnp.max(s, axis=1, keepdims=True)
        w = jnp.where(live, jnp.exp(s - peak), 0.0)
        total = jnp.sum(w, axis=1, keepdims=True)
        some = total > 0.0
        safe = jnp.where(some, total, 1.0)
        weights.append(w.astype(BF16))
        inverse.append(1.0 / safe)
        lse = jnp.where(some, peak + jnp.log(safe), very_low)
        lse_s[b : b + 1, :] = jnp.sum(jnp.where(eye, lse, 0.0), axis=0, keepdims=True)
    L["vc"].wait()
    for b in range(rows):
        part = mm(weights[b], vc[b]) * inverse[b]
        o_s[b : b + 1, :] = jnp.sum(jnp.where(head_mask, part, 0.0), axis=0, keepdims=True)
    lse_s[...] = jnp.where(lse_s[...] > very_low, lse_s[...] + (now_s[...] - base_s[...]), very_low)

    for d in reversed(kv_peers):
        arrived(EX_KV, kv_all, "kv", d)
    kv_here = jnp.sum(kv_all[...].astype(F32), axis=0)
    row_kv = lax.broadcasted_iota(jnp.int32, (rows, 2 * att), 0)
    kv_sum = jnp.zeros((rows, 2 * att), F32)
    for r in range(own_rows):
        kv_sum = jnp.where(row_kv == j * own_rows + r, kv_here[r : r + 1, :], kv_sum)
    kv_new = (row_scale * kv_sum).astype(BF16).astype(F32)
    product = q_s[...] * kv_new[:, 0:att]
    high = product.astype(BF16)
    low = (product - high.astype(F32)).astype(BF16)
    own_score = HEAD_DIM ** (-0.5) * (mm_t(high, spread) + mm_t(low, spread))
    owned = lax.broadcasted_iota(jnp.int32, (rows, LANES), 0) // own_rows == j
    own_score = jnp.where(owned, own_score, very_low)
    lse_old = lse_s[...]
    top = jnp.maximum(lse_old, own_score)
    part_old = jnp.where(lse_old > very_low, jnp.exp(lse_old - top), 0.0)
    part_new = jnp.where(owned, jnp.exp(own_score - top), 0.0)
    both = part_old + part_new
    some = both > 0.0
    both = jnp.where(some, both, 1.0)
    lse_all[j] = jnp.where(some, top + jnp.log(both), very_low)
    o_all[j] = (
        split_mm(part_old / both, spread) * o_s[...]
        + split_mm(part_new / both, spread) * kv_new[:, att:]
    ).astype(BF16)
    for d in kv_peers:
        send(EX_LSE, lse_all.at[j], lse_all.at[j], "kv", d, j)
        send(EX_O, o_all.at[j], o_all.at[j], "kv", d, j)
    for d in reversed(kv_peers):
        arrived(EX_LSE, lse_all, "kv", d)
    lse = lse_all[...]
    share = jnp.exp(lse - jnp.max(lse, axis=0, keepdims=True))
    share = share / jnp.sum(share, axis=0, keepdims=True)
    shares = split_mm(share.reshape(n_kv * rows, LANES), spread)
    for d in reversed(kv_peers):
        arrived(EX_O, o_all, "kv", d)
    attended = shares[0:rows] * o_all[0].astype(F32)
    for d in range(1, n_kv):
        attended += shares[d * rows : (d + 1) * rows] * o_all[d].astype(F32)
    attended = attended.astype(BF16)

    L["wo"].wait()
    out_all[t] = mm(attended, wo[...]).astype(BF16)
    for d in tp_peers:
        send(EX_OUT, out_all.at[t], out_all.at[t], "tp", d, t)
    for d in tp_peers:
        arrived(EX_OUT, out_all, "tp", d)
    head_terms = out_all[0].astype(F32)
    for d in range(1, n_tp):
        head_terms += out_all[d].astype(F32)
    mixed = (tokens_f + head_terms).astype(BF16).astype(F32)

    L["mg"].wait()
    mix_in = (mixed * mix_gain_v[...]).astype(BF16)
    sq_all[j] = jnp.broadcast_to(jnp.sum(mixed * mixed, axis=1, keepdims=True), (rows, LANES))
    for d in kv_peers:
        send(EX_SQ, sq_all.at[j], sq_all.at[j], "kv", d, j)
    L["wu"].wait()
    for d in kv_peers:
        up_send[d] = mm(mix_in, wu[:, pl.ds(pl.multiple_of(d * chunk, chunk), chunk)]).astype(BF16)
        send(EX_UP, up_send.at[d], up_all.at[j], "kv", d, j)
    up_all[j] = mm(mix_in, wu[:, pl.ds(pl.multiple_of(j * chunk, chunk), chunk)]).astype(BF16)
    for d in reversed(kv_peers):
        arrived(EX_SQ, sq_all, "kv", d)
    mix_scale = lax.rsqrt(jnp.sum(sq_all[...], axis=0)[:, 0:1] / width + epsilon)
    for d in reversed(kv_peers):
        arrived(EX_UP, up_all, "kv", d)
    upward = up_all[0].astype(F32)
    for d in range(1, n_kv):
        upward += up_all[d].astype(F32)
    act = jnp.maximum(mix_scale * upward, 0.0)
    hid_all[j] = (act * act).astype(BF16)
    for d in kv_peers:
        send(EX_HID, hid_all.at[j], hid_all.at[j], "kv", d, j)
    L["wd"].wait()

    def down(d):
        return mm(hid_all[d], wd[pl.ds(pl.multiple_of(d * chunk, chunk), chunk), :])

    total = down(j)
    for d in reversed(kv_peers):
        arrived(EX_HID, hid_all, "kv", d)
        total += down(d)
    down_all[t] = total.astype(BF16)
    for d in tp_peers:
        send(EX_DOWN, down_all.at[t], down_all.at[t], "tp", d, t)
    for d in tp_peers:
        arrived(EX_DOWN, down_all, "tp", d)
    channel = down_all[0].astype(F32)
    for d in range(1, n_tp):
        channel += down_all[d].astype(F32)
    out_h[...] = (mixed + channel).astype(BF16)
    for c in sent:
        c.wait_send()


def fast_shards(
    n_kv,
    n_tp,
    tokens,
    norm_gain,
    w_query,
    w_key,
    w_value,
    w_forget,
    w_out,
    mix_gain,
    w_up,
    w_down,
    key_cache,
    value_cache,
    decay_cache,
    lengths,
):
    rows, feats = tokens.shape
    att = w_query.shape[1]
    own_rows = rows // n_kv
    chunk = w_up.shape[1] // n_kv
    operands = (
        tokens,
        norm_gain.reshape(1, feats),
        w_query,
        w_key,
        w_value,
        w_forget.T,
        w_out,
        mix_gain.reshape(1, feats),
        w_up,
        w_down,
        key_cache,
        value_cache,
        decay_cache.transpose(1, 0, 2),
    )
    big = max(n_kv, n_tp)
    span = decay_cache.shape[2]
    scratch = [pltpu.VMEM(a.shape, a.dtype) for a in operands] + [
        pltpu.VMEM((n_kv, rows, att), BF16),
        pltpu.VMEM((n_kv, rows, LANES), F32),
        pltpu.VMEM((n_kv, own_rows, 2 * att), BF16),
        pltpu.VMEM((n_kv, own_rows, 2 * att), BF16),
        pltpu.VMEM((rows, att), F32),
        pltpu.VMEM((rows, decay_cache.shape[1], span), F32),
        pltpu.VMEM((rows, LANES), F32),
        pltpu.VMEM((rows, LANES), F32),
        pltpu.VMEM((rows, att), F32),
        pltpu.VMEM((rows, LANES), F32),
        pltpu.VMEM((n_kv, rows, att), BF16),
        pltpu.VMEM((n_kv, rows, LANES), F32),
        pltpu.VMEM((n_tp, rows, feats), BF16),
        pltpu.VMEM((n_kv, rows, chunk), BF16),
        pltpu.VMEM((n_kv, rows, chunk), BF16),
        pltpu.VMEM((n_kv, rows, LANES), F32),
        pltpu.VMEM((n_kv, rows, chunk), BF16),
        pltpu.VMEM((n_tp, rows, feats), BF16),
        pltpu.SemaphoreType.DMA((len(operands),)),
        pltpu.SemaphoreType.DMA((10, big)),
        pltpu.SemaphoreType.DMA((10, big)),
    ]
    return pl.pallas_call(
        functools.partial(layer_kernel, n_kv, n_tp),
        out_shape=jax.ShapeDtypeStruct(tokens.shape, tokens.dtype),
        in_specs=[pl.BlockSpec(memory_space=pltpu.SMEM)]
        + [pl.BlockSpec(memory_space=pl.ANY)] * len(operands),
        out_specs=pl.BlockSpec(memory_space=pltpu.VMEM),
        scratch_shapes=scratch,
        compiler_params=pltpu.CompilerParams(
            collective_id=0, has_side_effects=True, vmem_limit_bytes=56 * 1024 * 1024
        ),
    )(lengths, *operands)


def local_softmax(query_heads, score_bias, keys_block, values_block, live_mask):
    rows_count, count = (keys_block.shape[0], keys_block.shape[1])
    heads_count = query_heads.shape[1]
    keys_view = keys_block.reshape(rows_count, count, heads_count, HEAD_DIM)
    values_view = values_block.reshape(rows_count, count, heads_count, HEAD_DIM)
    scores = jnp.einsum("bhe,bphe->bhp", query_heads, keys_view, preferred_element_type=jnp.float32)
    scores = scores * HEAD_DIM ** (-0.5) + score_bias
    block_peak = jnp.max(jnp.where(live_mask, scores, very_low), axis=2)
    weights = jnp.where(live_mask, jnp.exp(scores - block_peak[..., None]), 0.0)
    totals = jnp.sum(weights, axis=2)
    weighted = jnp.einsum(
        "bhp,bphe->bhe",
        weights.astype(jnp.bfloat16),
        values_view,
        preferred_element_type=jnp.float32,
    )
    return (block_peak, totals, weighted)


def shards(
    tokens,
    norm_gain,
    w_query,
    w_key,
    w_value,
    w_forget,
    w_out,
    mix_gain,
    w_up,
    w_down,
    key_cache,
    value_cache,
    decay_cache,
    lengths,
):
    rows_count = tokens.shape[0]
    width = tokens.shape[1] * lax.axis_size("kv")
    heads_here = decay_cache.shape[1]
    span = key_cache.shape[1]
    tokens_f = tokens.astype(jnp.float32)
    scaled_in = (tokens_f * norm_gain).astype(jnp.bfloat16)
    forget_cols = lax.dynamic_slice_in_dim(
        w_forget, lax.axis_index("tp") * heads_here, heads_here, 1
    )
    positions = lax.axis_index("kv") * span + jnp.arange(span, dtype=jnp.int32)
    newest = positions[None, None, :] == (lengths - 1)[:, None, None]
    summed = lax.psum(
        (
            jnp.dot(scaled_in, w_query, preferred_element_type=jnp.float32),
            jnp.dot(scaled_in, w_key, preferred_element_type=jnp.float32),
            jnp.dot(scaled_in, w_value, preferred_element_type=jnp.float32),
            jnp.dot(scaled_in, forget_cols, preferred_element_type=jnp.float32),
            jnp.sum(tokens_f * tokens_f, axis=1),
            jnp.sum(jnp.where(newest, decay_cache, 0.0), axis=2),
        ),
        "kv",
    )
    row_scale = lax.rsqrt(summed[4] / width + epsilon)[:, None]
    queries = (row_scale * summed[0]).astype(jnp.bfloat16)
    new_keys = (row_scale * summed[1]).astype(jnp.bfloat16)
    new_values = (row_scale * summed[2]).astype(jnp.bfloat16)
    now_decay = summed[5] + jax.nn.log_sigmoid(row_scale * summed[3])
    query_heads = queries.reshape(rows_count, heads_here, HEAD_DIM)
    own_score = jnp.sum(
        query_heads.astype(jnp.float32)
        * new_keys.astype(jnp.float32).reshape(rows_count, heads_here, HEAD_DIM),
        axis=2,
    ) * HEAD_DIM ** (-0.5)
    own_values = new_values.astype(jnp.float32).reshape(rows_count, heads_here, HEAD_DIM)
    live_mask = positions[None, None, :] < lengths[:, None, None]
    local_state = local_softmax(
        query_heads, now_decay[:, :, None] - decay_cache, key_cache, value_cache, live_mask
    )
    global_peak = lax.pmax(local_state[0], "kv")
    highest = jnp.maximum(global_peak, own_score)
    factor_here = jnp.exp(local_state[0] - highest)
    total_sum, weighted_sum = lax.psum(
        (local_state[1] * factor_here, local_state[2] * factor_here[..., None]), "kv"
    )
    factor_own = jnp.exp(own_score - highest)
    final_state = (
        highest,
        total_sum + factor_own,
        weighted_sum + factor_own[..., None] * own_values,
    )
    attended = (
        (final_state[2] / final_state[1][..., None])
        .reshape(rows_count, heads_here * HEAD_DIM)
        .astype(jnp.bfloat16)
    )
    head_terms = lax.psum(jnp.dot(attended, w_out, preferred_element_type=jnp.float32), "tp")
    mixed_f = (tokens_f + head_terms).astype(jnp.bfloat16).astype(jnp.float32)
    mix_in = (mixed_f * mix_gain).astype(jnp.bfloat16)
    up_terms = jnp.dot(mix_in, w_up, preferred_element_type=jnp.float32)
    squares_here = jnp.sum(mixed_f * mixed_f, axis=1)
    upward, squares_all = lax.psum((up_terms, squares_here), "kv")
    mix_scale = lax.rsqrt(squares_all / width + epsilon)[:, None]
    hidden = (jax.nn.relu(mix_scale * upward) ** 2).astype(jnp.bfloat16)
    down_terms = jnp.dot(hidden, w_down, preferred_element_type=jnp.float32)
    channel_terms = lax.psum(down_terms, "tp")
    return (mixed_f + channel_terms).astype(jnp.bfloat16)


def fits(n_kv, *operands):
    tokens, w_query, w_up, decay = (operands[0], operands[2], operands[8], operands[12])
    rows, feats = tokens.shape
    return (
        rows % n_kv == 0
        and feats % LANES == 0
        and w_query.shape[1] % LANES == 0
        and w_up.shape[1] % (n_kv * LANES) == 0
        and decay.shape[2] % LANES == 0
        and decay.shape[1] <= LANE_NEWEST
    )


def solution(mesh):
    placed = (
        P(None, "kv"),
        P("kv"),
        P("kv", "tp"),
        P("kv", "tp"),
        P("kv", "tp"),
        P("kv", None),
        P("tp", "kv"),
        P("kv"),
        P("kv", "tp"),
        P("tp", "kv"),
        P(None, "kv", "tp"),
        P(None, "kv", "tp"),
        P(None, "tp", "kv"),
        P(),
    )
    n_kv, n_tp = mesh.shape["kv"], mesh.shape["tp"]

    def layer(*operands):
        body = functools.partial(fast_shards, n_kv, n_tp) if fits(n_kv, *operands) else shards
        return body(*operands)

    return jax.shard_map(
        layer, mesh=mesh, in_specs=placed, out_specs=P(None, "kv"), check_vma=False
    )
```
